32 devices in a mesh: sp: 8 (over z, core), tp: 4 (over y, x).
Axes of the slice: x: 2, y: 2, z: 4, core: 2. Of those that a mesh axis runs over, the one named last changes fastest.
Arguments:
- tokens: bfloat16 [1536, 4096], P('sp', 'tp'), may hold values from -60 to 60
- lean_query: bfloat16 [1536, 16, 64], P('sp', 'tp'), may hold values from -6 to 6
- lean_key: bfloat16 [1536, 2, 64], P('sp'), may hold values from -6 to 6
- lean_value: bfloat16 [1536, 2, 64], P('sp'), may hold values from -6 to 6
- lean_gains: float32 [2, 64], replicated, may hold values from 0.25 to 7.5
- broad_query: bfloat16 [1536, 16, 128], P('sp', 'tp'), may hold values from -6 to 6
- broad_key: bfloat16 [1536, 2, 128], P('sp'), may hold values from -6 to 6
- broad_value: bfloat16 [1536, 2, 128], P('sp'), may hold values from -6 to 6
- broad_gains: float32 [2, 128], replicated, may hold values from 0.25 to 7.5
- mixer_gain: float32 [3072], replicated, may hold values from 0.1 to 1.9
- output_weight: bfloat16 [3072, 4096], P(None, 'tp'), may hold values from -0.109375 to 0.109375
- channel_gain: float32 [4096], P('tp'), may hold values from 0.1 to 1.9
- gate_weight: bfloat16 [8, 4096, 2048], P('sp', None, 'tp'), may hold values from -0.09375 to 0.09375
- up_weight: bfloat16 [8, 4096, 2048], P('sp', None, 'tp'), may hold values from -0.09375 to 0.09375
- down_weight: bfloat16 [8, 2048, 4096], P('sp', None, 'tp'), may hold values from -0.125 to 0.125
- route_experts: int32 [1536, 2], P('sp'), may hold values from 0 to 7, as said below
- route_logits: float32 [1536, 2], P('sp'), may hold values from -6 to 6
- group_weight: float32 [1536], P('sp'), may hold values from 0.3 to 1
Outputs:
- encoded: bfloat16 [1536, 4096], P('sp', 'tp')
The draws below stay inside these ranges and needn't reach their ends.
Inputs may be any that keep to these rules, and one draw needn't show every extreme that they name: `route_experts`: each row names two different experts of one group, expert e lying in group e // 2. In every aligned block of 192 rows no expert is named by more than 96 rows; one group, the same for all blocks, is named by exactly half of each block's rows, and each of its experts by exactly 96 of them.
All inputs are finite; a program needn't handle non-finite values.
Results may differ from the reference program's by a relative error of at most 0.0083.
Values may be sent and summed in bfloat16 or wider, within the bound.
A program may use at most 64 MiB of HBM per device.

```python
import jax
import jax.numpy as jnp
from jax import lax

TOK_SP = 192
SEQ = 1536
D = 4096
HQ_A = 16
KV_A = 2
HD_A = 64
HQ_B = 16
KV_B = 2
HD_B = 128
DMIX = 3072
GRID_W = 64
EXPERTS = 8
GROUPS = 4
EPG = 2
TOPK = 2
FF = 2048
CAP = 96
N_SP = 8


def drawn_pair(base_key, head_count, key_heads, head_size):
    subkeys = jax.random.split(base_key, 2)
    keys = jax.random.normal(subkeys[0], (SEQ, key_heads, head_size), jnp.float32)
    queries = jax.random.normal(subkeys[1], (SEQ, head_count, head_size), jnp.float32)
    return (jnp.clip(queries, -6.0, 6.0), jnp.clip(keys, -6.0, 6.0))


def gain_draw(base_key, head_size):
    return 1.0 + 0.18 * jnp.clip(jax.random.normal(base_key, (2, head_size), jnp.float32), -4.0, 4.0)


def draw_lean_query(key, part):
    return drawn_pair(jax.random.fold_in(key, 101), HQ_A, KV_A, HD_A)[0].astype(jnp.bfloat16)


def draw_lean_key(key, part):
    return drawn_pair(jax.random.fold_in(key, 101), HQ_A, KV_A, HD_A)[1].astype(jnp.bfloat16)


def draw_broad_query(key, part):
    return drawn_pair(jax.random.fold_in(key, 102), HQ_B, KV_B, HD_B)[0].astype(jnp.bfloat16)


def draw_broad_key(key, part):
    return drawn_pair(jax.random.fold_in(key, 102), HQ_B, KV_B, HD_B)[1].astype(jnp.bfloat16)


def draw_lean_gains(key, part):
    return gain_draw(jax.random.fold_in(key, 201), HD_A)


def draw_broad_gains(key, part):
    return gain_draw(jax.random.fold_in(key, 202), HD_B)


def draw_tokens(key, part):
    first_key, second_key = jax.random.split(jax.random.fold_in(key, 401))
    column = jnp.arange(D, dtype=jnp.float32) / D
    base_values = jnp.clip(jax.random.normal(first_key, (SEQ, D), jnp.float32), -5.0, 5.0)
    column_scale = 0.3 * 10.0 ** column
    row_scale = 0.4 * 10.0 ** jax.random.uniform(second_key, (SEQ, 1), jnp.float32)
    return (base_values * column_scale[None, :] * row_scale).astype(jnp.bfloat16)


def draw_route_experts(key, part):
    block_count = SEQ // TOK_SP
    half_rows = TOK_SP // 2
    big_group = jax.random.randint(jax.random.fold_in(key, 7), (), 0, GROUPS)
    block_keys = jax.random.split(jax.random.fold_in(key, 11), block_count)

    def one_block(block_key):
        cut_key, order_key, rank_key, inner_key = jax.random.split(block_key, 4)
        cut_points = jnp.sort(jax.random.randint(cut_key, (GROUPS - 2,), 0, half_rows + 1))
        bounds = jnp.concatenate([jnp.zeros((1,), jnp.int32), cut_points, jnp.full((1,), half_rows, jnp.int32)])
        starts = jnp.concatenate([jnp.zeros((1,), jnp.int32), half_rows + bounds[:-1]])
        ends = jnp.concatenate([jnp.full((1,), half_rows, jnp.int32), half_rows + bounds[1:]])
        others = (big_group + 1 + jax.random.permutation(order_key, GROUPS - 1)) % GROUPS
        group_order = jnp.concatenate([big_group[None], others])
        token_rank = jax.random.permutation(rank_key, TOK_SP)
        member = ((token_rank[:, None] >= starts[None, :]) & (token_rank[:, None] < ends[None, :])).astype(jnp.int32)
        which = jnp.argmax(member, axis=1)
        chosen_group = group_order[which]
        inner = token_rank - starts[which]
        first_pick = inner % EPG
        second_pick = (inner + 1 + inner // EPG % (EPG - 1)) % EPG
        shuffles = jax.vmap(lambda each_key: jax.random.permutation(each_key, EPG))(jax.random.split(inner_key, GROUPS))
        first_expert = chosen_group * EPG + shuffles[chosen_group, first_pick]
        second_expert = chosen_group * EPG + shuffles[chosen_group, second_pick]
        return jnp.stack([first_expert, second_expert], axis=1)
    return jax.vmap(one_block)(block_keys).reshape(SEQ, TOPK).astype(jnp.int32)


def shard_levels(rng, dims, pieces, low, high):
    loudness = 1.0
    for position, parts in pieces:
        draws = jax.random.uniform(jax.random.fold_in(jax.random.fold_in(rng, 6), position), (parts,), jnp.float32, low / len(pieces), high / len(pieces))
        loudness = loudness * jnp.repeat(jnp.exp(draws), dims[position] // parts).reshape((-1,) + (1,) * (len(dims) - 1 - position))
    return loudness


def gaussian(own_key, dims, spread, limit, cuts=(), kind=jnp.bfloat16):
    values = spread * jax.random.normal(own_key, dims, jnp.float32)
    if cuts:
        values = values * shard_levels(own_key, dims, cuts, -0.22, 0.18)
    return jnp.clip(values, -limit, limit).astype(kind)


def setup_inputs(seed: int = 0) -> dict:
    splits = jax.random.split(jax.random.key(seed), 19)
    return {
        "tokens": draw_tokens(jax.random.fold_in(splits[18], 71), 0),
        "lean_query": draw_lean_query(jax.random.fold_in(splits[18], 71), 0),
        "lean_key": draw_lean_key(jax.random.fold_in(splits[18], 71), 0),
        "lean_value": gaussian(splits[3], (SEQ, KV_A, HD_A), 1.0, 6.0, ((0, 8),)),
        "lean_gains": draw_lean_gains(jax.random.fold_in(splits[18], 71), 0),
        "broad_query": draw_broad_query(jax.random.fold_in(splits[18], 71), 0),
        "broad_key": draw_broad_key(jax.random.fold_in(splits[18], 71), 0),
        "broad_value": gaussian(splits[7], (SEQ, KV_B, HD_B), 1.0, 6.0, ((0, 8),)),
        "broad_gains": draw_broad_gains(jax.random.fold_in(splits[18], 71), 0),
        "mixer_gain": jnp.clip(1.0 + 0.18 * jax.random.normal(splits[9], (DMIX,), jnp.float32), 0.1, 1.9),
        "output_weight": gaussian(splits[10], (DMIX, D), DMIX ** -0.5, 0.109375, ((1, 4),)),
        "channel_gain": jnp.clip(1.0 + 0.18 * jax.random.normal(splits[11], (D,), jnp.float32), 0.1, 1.9),
        "gate_weight": gaussian(splits[12], (EXPERTS, D, FF), D ** -0.5, 0.09375, ((0, 8), (2, 4))),
        "up_weight": gaussian(splits[13], (EXPERTS, D, FF), D ** -0.5, 0.09375, ((0, 8), (2, 4))),
        "down_weight": gaussian(splits[14], (EXPERTS, FF, D), FF ** -0.5, 0.125, ((0, 8), (2, 4))),
        "route_experts": draw_route_experts(jax.random.fold_in(splits[18], 71), 0),
        "route_logits": gaussian(splits[16], (SEQ, TOPK), 1.5, 6.0, ((0, 8),), jnp.float32),
        "group_weight": jnp.clip(0.3 + 0.7 * jax.random.uniform(splits[17], (SEQ,), jnp.float32) ** shard_levels(splits[17], (SEQ,), ((0, 8),), -0.2, 0.2), 0.3, 1.0),
    }


epsilon = 1e-06
theta_base = 10000.0

def axial_angles(positions, head_size):
    quarter = head_size // 4
    frequency = theta_base ** (-jnp.arange(quarter, dtype=jnp.float32) / quarter)
    grid_rows = (positions // GRID_W).astype(jnp.float32)
    grid_columns = (positions % GRID_W).astype(jnp.float32)
    return (grid_rows[:, None] * frequency[None, :], grid_columns[:, None] * frequency[None, :])

def turn_half(values, angles):
    half_width = values.shape[-1] // 2
    first_half = values[..., :half_width]
    second = values[..., half_width:]
    cosine = jnp.cos(angles)[:, None, :]
    sine_part = jnp.sin(angles)[:, None, :]
    return jnp.concatenate([first_half * cosine - second * sine_part, second * cosine + first_half * sine_part], axis=-1)

def prepare(raw_values, gain_row, positions):
    values = raw_values.astype(jnp.float32)
    values = values * lax.rsqrt(lax.optimization_barrier(jnp.mean(values * values, axis=-1, keepdims=True)) + epsilon) * gain_row
    row_angles, column_angles = axial_angles(positions, raw_values.shape[-1])
    half_width = raw_values.shape[-1] // 2
    turned = jnp.concatenate([turn_half(values[..., :half_width], row_angles), turn_half(values[..., half_width:], column_angles)], axis=-1)
    return turned.astype(jnp.bfloat16)

def attend(queries, keys, values):
    token_count, head_count, head_size = queries.shape
    key_heads = keys.shape[1]
    group_ratio = head_count // key_heads
    blocks = queries.reshape(token_count // TOK_SP, TOK_SP, key_heads, group_ratio, head_size)
    keys_wide = keys.astype(jnp.float32)
    values_wide = values.astype(jnp.float32)

    def one_block(block_queries):
        scores = jnp.einsum('qkgd,skd->kgqs', block_queries.astype(jnp.float32), keys_wide) * head_size ** (-0.5)
        peak_score = lax.optimization_barrier(jnp.max(scores, axis=-1, keepdims=True))
        weights = jnp.exp(scores - peak_score)
        weight_sum = lax.optimization_barrier(jnp.sum(weights, axis=-1))
        rounded = lax.optimization_barrier(weights.astype(jnp.bfloat16)).astype(jnp.float32)
        summed = jnp.einsum('kgqs,skd->qkgd', rounded, values_wide)
        return (summed / jnp.transpose(weight_sum, (2, 0, 1))[..., None]).astype(jnp.bfloat16)
    mixed_heads = lax.map(one_block, blocks)
    return mixed_heads.reshape(token_count, head_count * head_size)

def group_norm(head_rows, gain_row):
    values = head_rows.astype(jnp.float32)
    return (values * lax.rsqrt(lax.optimization_barrier(jnp.mean(values * values, axis=-1, keepdims=True)) + epsilon) * gain_row).astype(jnp.bfloat16)

def reference(tokens, lean_query, lean_key, lean_value, lean_gains, broad_query, broad_key, broad_value, broad_gains, mixer_gain, output_weight, channel_gain, gate_weight, up_weight, down_weight, route_experts, route_logits, group_weight):
    positions = jnp.arange(SEQ, dtype=jnp.int32)
    lean_out = attend(prepare(lean_query, lean_gains[0], positions), prepare(lean_key, lean_gains[1], positions), lean_value)
    broad_out = attend(prepare(broad_query, broad_gains[0], positions), prepare(broad_key, broad_gains[1], positions), broad_value)
    lean_width = HQ_A * HD_A
    mixed_rows = jnp.concatenate([group_norm(lean_out, mixer_gain[:lean_width]), group_norm(broad_out, mixer_gain[lean_width:])], axis=1)
    stream = tokens.astype(jnp.float32) + jnp.dot(mixed_rows, output_weight, preferred_element_type=jnp.float32)
    normed = (stream * lax.rsqrt(lax.optimization_barrier(jnp.mean(stream * stream, axis=-1, keepdims=True)) + epsilon) * channel_gain).astype(jnp.bfloat16)
    logit_gap = route_logits[:, 0] - route_logits[:, 1]
    weights = group_weight[:, None] * jax.nn.sigmoid(jnp.stack([logit_gap, -logit_gap], axis=1))
    row_bound = N_SP * CAP

    def one_expert(running, expert_index):
        hit_mask = route_experts == expert_index
        member = jnp.any(hit_mask, axis=1)
        chosen = jnp.nonzero(member, size=row_bound, fill_value=0)[0]
        valid_rows = (jnp.arange(row_bound) < jnp.sum(member.astype(jnp.int32))).astype(jnp.float32)
        picked = normed[chosen]
        gate_value = jnp.dot(picked, gate_weight[expert_index], preferred_element_type=jnp.float32)
        up_value = jnp.dot(picked, up_weight[expert_index], preferred_element_type=jnp.float32)
        hidden = (jax.nn.silu(gate_value) * up_value).astype(jnp.bfloat16)
        result = jnp.dot(hidden, down_weight[expert_index], preferred_element_type=jnp.float32).astype(jnp.bfloat16)
        coefficient = lax.optimization_barrier(jnp.sum(jnp.where(hit_mask, weights, 0.0), axis=1))[chosen] * valid_rows
        return (running.at[chosen].add(coefficient[:, None] * result.astype(jnp.float32)), None)
    routed = lax.scan(one_expert, jnp.zeros((SEQ, D), jnp.float32), jnp.arange(EXPERTS, dtype=jnp.int32))[0]
    return (stream + routed).astype(jnp.bfloat16)
```

```python
import functools

import jax
import jax.numpy as jnp
import numpy as np
from jax import lax
from jax.experimental import pallas as pl
from jax.experimental.pallas import tpu as pltpu
from jax.sharding import PartitionSpec as P

D = 4096
HQ_A = 16
KV_A = 2
HQ_B = 16
KV_B = 2
GRID_W = 64
GROUPS = 4


epsilon = 1e-06
theta_base = 10000.0
floor_score = -1e30


def axial_angles(positions, head_size):
    quarter = head_size // 4
    frequency = theta_base ** (-jnp.arange(quarter, dtype=jnp.float32) / quarter)
    grid_rows = (positions // GRID_W).astype(jnp.float32)
    grid_columns = (positions % GRID_W).astype(jnp.float32)
    return (grid_rows[:, None] * frequency[None, :], grid_columns[:, None] * frequency[None, :])


def turn_half(values, angles):
    half_width = values.shape[-1] // 2
    first_half = values[..., :half_width]
    second = values[..., half_width:]
    cosine = jnp.cos(angles)[:, None, :]
    sine_part = jnp.sin(angles)[:, None, :]
    return jnp.concatenate(
        [first_half * cosine - second * sine_part, second * cosine + first_half * sine_part],
        axis=-1,
    )


def prepare(raw_values, gain_row, positions):
    values = raw_values.astype(jnp.float32)
    values = (
        values * lax.rsqrt(jnp.mean(values * values, axis=-1, keepdims=True) + epsilon) * gain_row
    )
    row_angles, column_angles = axial_angles(positions, raw_values.shape[-1])
    half_width = raw_values.shape[-1] // 2
    turned = jnp.concatenate(
        [
            turn_half(values[..., :half_width], row_angles),
            turn_half(values[..., half_width:], column_angles),
        ],
        axis=-1,
    )
    return turned.astype(jnp.bfloat16)


def group_norm(head_rows, gain_row):
    values = head_rows.astype(jnp.float32)
    return (
        values * lax.rsqrt(jnp.mean(values * values, axis=-1, keepdims=True) + epsilon) * gain_row
    ).astype(jnp.bfloat16)


def own_heads(query_raw, key_raw, value_raw, gain_pair, positions, lane_index, group_ratio):
    head_count, head_size = (query_raw.shape[1], query_raw.shape[2])
    key_heads = max(1, head_count // group_ratio)
    kv_start = lane_index * head_count // group_ratio
    key_part = lax.dynamic_slice_in_dim(key_raw, kv_start, key_heads, 1)
    value_part = lax.dynamic_slice_in_dim(value_raw, kv_start, key_heads, 1)
    queries = prepare(query_raw, gain_pair[0], positions).reshape(
        query_raw.shape[0], key_heads, head_count // key_heads, head_size
    )
    return (queries, prepare(key_part, gain_pair[1], positions), value_part)


def start_state(queries):
    row_count = queries.shape[0]
    head_count = queries.shape[1] * queries.shape[2]
    return (
        jnp.full((head_count, row_count), floor_score, jnp.float32),
        jnp.zeros((head_count, row_count), jnp.float32),
        jnp.zeros((row_count, head_count, queries.shape[3]), jnp.float32),
    )


def attend_piece(fold_state, queries, keys, values):
    peak_score, weight_sum, accumulated = fold_state
    row_count, key_heads, grouped, head_size = queries.shape
    key_count = keys.shape[0]
    scores = jnp.einsum(
        "qkgd,skd->kgqs", queries, keys, preferred_element_type=jnp.float32
    ) * head_size ** (-0.5)
    scores = scores.reshape(key_heads * grouped, row_count, key_count)
    new_peak = jnp.maximum(peak_score, jnp.max(scores, axis=-1))
    weights = jnp.exp(scores - new_peak[..., None])
    new_sum = jnp.sum(weights, axis=-1)
    rounded = weights.astype(jnp.bfloat16).reshape(key_heads, grouped, row_count, key_count)
    partial_value = jnp.einsum(
        "kgqs,skd->qkgd", rounded, values, preferred_element_type=jnp.float32
    )
    partial_value = partial_value.reshape(row_count, key_heads * grouped, head_size)
    return (new_peak, new_sum, partial_value)


def finish_heads(fold_state):
    accumulated = fold_state[2]
    return (
        (accumulated / jnp.transpose(fold_state[1])[:, :, None])
        .astype(jnp.bfloat16)
        .reshape(accumulated.shape[0], -1)
    )


MESH = pl.DeviceIdType.MESH
COPIES = 160
LOG2E = 1.4426950408889634


def remote(source, target, send_sem, recv_sem, device):
    return pltpu.make_async_remote_copy(
        src_ref=source,
        dst_ref=target,
        send_sem=send_sem,
        recv_sem=recv_sem,
        device_id=device,
        device_id_type=MESH,
    )


def eye(size, dtype):
    rows = lax.broadcasted_iota(jnp.int32, (size, size), 0)
    columns = lax.broadcasted_iota(jnp.int32, (size, size), 1)
    return jnp.where(rows == columns, 1.0, 0.0).astype(dtype)


def to_column(row):
    size = row.shape[1]
    rows = lax.broadcasted_iota(jnp.int32, (size, size), 0)
    columns = lax.broadcasted_iota(jnp.int32, (size, size), 1)
    spread = jnp.broadcast_to(row, (size, size))
    return jnp.sum(jnp.where(rows == columns, spread, 0.0), axis=1, keepdims=True)


def to_row(column):
    size = column.shape[0]
    rows = lax.broadcasted_iota(jnp.int32, (size, size), 0)
    columns = lax.broadcasted_iota(jnp.int32, (size, size), 1)
    spread = jnp.broadcast_to(column, (size, size))
    return jnp.sum(jnp.where(rows == columns, spread, 0.0), axis=0, keepdims=True)


def dot_nt(left, right):
    return lax.dot_general(
        left, right, (((1,), (1,)), ((), ())), preferred_element_type=jnp.float32
    )


def layer_kernel(
    chips,
    lean_q_hbm,
    lean_k_hbm,
    lean_v_hbm,
    broad_q_hbm,
    broad_k_hbm,
    broad_v_hbm,
    lean_gain_hbm,
    broad_gain_hbm,
    lean_rows_hbm,
    lean_columns_hbm,
    broad_rows_hbm,
    broad_columns_hbm,
    experts_hbm,
    logits_hbm,
    group_hbm,
    mixer_hbm,
    tokens_hbm,
    channel_hbm,
    weight_hbm,
    gate_hbm,
    up_hbm,
    down_hbm,
    out_ref,
    lean_q,
    lean_k,
    lean_v,
    broad_q,
    broad_k,
    broad_v,
    lean_gain,
    broad_gain,
    lean_rows,
    lean_columns,
    broad_rows,
    broad_columns,
    experts,
    logits,
    group_weight,
    mixer_gain,
    tokens,
    channel_gain,
    weight,
    gate_w,
    up_w,
    down_w,
    pairs_f32,
    own,
    keys,
    queries,
    peak,
    total,
    lean_mass,
    broad_mass,
    lean_heads,
    broad_heads,
    lean_acc,
    broad_acc,
    stream,
    scaled,
    picker,
    unpicker,
    routes,
    norms,
    extras,
    going,
    rows,
    gate_acc,
    up_acc,
    hidden,
    result,
    swap_send,
    swap_recv,
    back,
    arrived,
    load_sem,
    send_sem,
    recv_sem,
):
    sp, tp = lax.axis_index("sp"), lax.axis_index("tp")
    z, core = sp // 2, sp % 2
    y, x = tp // 2, tp % 2
    sibling = {"sp": z * 2 + (1 - core), "tp": tp}
    x_peer = {"sp": sp, "tp": y * 2 + (1 - x)}
    y_peer = {"sp": sp, "tp": (1 - y) * 2 + x}
    far_peer = {"sp": sp, "tp": (1 - y) * 2 + (1 - x)}
    chunks = (tp, y * 2 + (1 - x), (1 - y) * 2 + x, (1 - y) * 2 + (1 - x))
    ahead = [{"sp": ((z + d) % chips) * 2 + core, "tp": tp} for d in range(chips)]
    behind = [{"sp": ((z + chips - d) % chips) * 2 + core, "tp": tp} for d in range(chips)]
    peers = ahead[1:] + [sibling, x_peer, y_peer, far_peer]
    barrier = pltpu.get_barrier_semaphore()
    for peer in peers:
        pl.semaphore_signal(barrier, inc=1, device_id=peer, device_id_type=MESH)

    count = own.shape[0]
    half = count // 2
    cap = count // 2
    lanes = 128
    width = tokens.shape[1]
    heads = lean_q.shape[0]
    tile = count
    tiles = heads

    loads = []

    def load(source, target):
        copy = pltpu.make_async_copy(source, target, load_sem.at[len(loads)])
        copy.start()
        loads.append(copy)
        return copy

    first_loads = [
        load(broad_k_hbm, broad_k),
        load(broad_v_hbm, broad_v),
        load(lean_k_hbm, lean_k),
        load(lean_v_hbm, lean_v),
        load(lean_gain_hbm, lean_gain),
        load(broad_gain_hbm, broad_gain),
        load(lean_rows_hbm.at[sp], lean_rows),
        load(lean_columns_hbm, lean_columns),
        load(broad_rows_hbm.at[sp], broad_rows),
        load(broad_columns_hbm, broad_columns),
    ]
    query_loads = [load(broad_q_hbm, broad_q), load(lean_q_hbm, lean_q)]
    route_loads = [
        load(experts_hbm, experts),
        load(logits_hbm, logits),
        load(group_hbm, group_weight),
        load(mixer_hbm, mixer_gain),
        load(tokens_hbm, tokens),
        load(channel_hbm, channel_gain),
    ]
    weight_load = load(weight_hbm, weight)
    gate_loads = [load(gate_hbm, gate_w), load(up_hbm, up_w)]
    down_load = load(down_hbm, down_w)

    pending = []
    arrivals = {}

    def send(key, source, target, device):
        n = len(pending)
        copy = remote(source, target, send_sem.at[n], recv_sem.at[n], device)
        copy.start()
        pending.append(copy)
        arrivals[key] = copy

    def arrive(*key):
        arrivals[key].wait_recv()

    unit = eye(count, jnp.bfloat16)

    def broad_turned(raw, gain, columns, row_values):
        values = raw.astype(jnp.float32)
        mean = jnp.sum(values * values, axis=1, keepdims=True) / lanes
        values = values * lax.rsqrt(mean + epsilon) * gain
        quarter = lanes // 4
        lane = lax.broadcasted_iota(jnp.int32, values.shape, 1)
        partner = jnp.where(
            lane % (2 * quarter) < quarter,
            pltpu.roll(values, lanes - quarter, 1),
            pltpu.roll(values, quarter, 1),
        )
        cosine = columns[0] + row_values[:, :lanes]
        sine = columns[1] + row_values[:, lanes:]
        return values * cosine + partner * sine

    def lean_turned(raw, gain):
        values = raw.astype(jnp.float32)
        size = values.shape[0]
        quarter = size // 4
        mean = jnp.sum(values * values, axis=0, keepdims=True) / size
        values = values * lax.rsqrt(mean + epsilon) * gain
        turned = []
        for start, table in ((0, lean_rows), (size // 2, lean_columns)):
            u = values[start : start + quarter]
            w = values[start + quarter : start + 2 * quarter]
            cosine, sine = table[:quarter], table[quarter:]
            turned += [u * cosine - w * sine, w * cosine + u * sine]
        return jnp.concatenate(turned, axis=0)

    for copy in first_loads:
        copy.wait()
    key_heads = lean_k.shape[0]
    pairs_f32[0] = broad_k[...].astype(jnp.float32)
    pairs_f32[1] = broad_v[...].astype(jnp.float32)
    grid_rows = broad_rows.shape[0]
    run = count // grid_rows
    for i in range(grid_rows):
        part = pl.ds(i * run, run)
        picked = pl.ds(y + i * run * key_heads, run, stride=key_heads)
        columns = [broad_columns[k, pl.ds(0, run, stride=heads), :] for k in range(2)]
        own[part, :lanes] = broad_turned(
            pairs_f32[0, picked, :], broad_gain[1:2, :], columns, broad_rows[i : i + 1, :]
        ).astype(jnp.bfloat16)
        own[part, lanes : 2 * lanes] = pairs_f32[1, picked, :].astype(jnp.bfloat16)
    size = lean_k.shape[1]
    lean_pair = jnp.concatenate(
        [lean_turned(lean_k[y], to_column(lean_gain[1:2, :])).astype(jnp.bfloat16), lean_v[y]],
        axis=0,
    )
    own[:, 2 * lanes :] = dot_nt(unit, lean_pair).astype(jnp.bfloat16)

    pl.semaphore_wait(barrier, len(peers))
    mine = pl.ds(pl.multiple_of(x * half, half), half)
    other = pl.ds(pl.multiple_of((1 - x) * half, half), half)
    side_mine = pl.ds(pl.multiple_of(count + x * half, half), half)
    side_other = pl.ds(pl.multiple_of(count + (1 - x) * half, half), half)
    for d in range(1, chips):
        send(("kz", d), own.at[mine], keys.at[d, mine], ahead[d])
    send(("ka", 0), own, keys.at[0, pl.ds(count, count)], sibling)
    keys[0, pl.ds(0, count)] = own[...]

    for copy in query_loads:
        copy.wait()
    q_run = run * heads
    for i in range(grid_rows):
        part = pl.ds(i * q_run, q_run)
        queries[1, part] = broad_turned(
            broad_q[part, :], broad_gain[0:1, :], broad_columns, broad_rows[i : i + 1, :]
        ).astype(jnp.bfloat16)
    query_gain = to_column(lean_gain[0:1, :])
    blank = jnp.zeros((lanes - size, count), jnp.bfloat16)
    for h in range(heads):
        turned = lean_turned(lean_q[h], query_gain).astype(jnp.bfloat16)
        queries[0, pl.ds(h * count, count)] = dot_nt(
            unit, jnp.concatenate([turned, blank], axis=0)
        ).astype(jnp.bfloat16)

    def attend(d, kind, start, stop):
        head_size = size if kind == 0 else lanes
        scale = head_size ** (-0.5) * LOG2E
        key_part = pl.ds(2 * lanes, lanes) if kind == 0 else pl.ds(0, lanes)
        value_part = pl.ds(2 * lanes, lanes) if kind == 0 else pl.ds(lanes, lanes)
        mass = lean_mass if kind == 0 else broad_mass

        def one_tile(i):
            part = pl.ds(pl.multiple_of(i * tile, tile), tile)
            scores = dot_nt(queries[kind, part], keys[d, :, key_part])
            top = jnp.max(scores, axis=1, keepdims=True)
            if d:
                old = peak[kind, part][:, :1]
                top = jnp.maximum(old, top)
            weights = jnp.exp2((scores - top) * scale)
            summed = jnp.sum(weights, axis=1, keepdims=True)
            partial = jnp.dot(
                weights.astype(jnp.bfloat16),
                keys[d, :, value_part],
                preferred_element_type=jnp.float32,
            )
            if d:
                shrink = jnp.exp2((old - top) * scale)
                summed = summed + total[kind, part][:, :1] * shrink
                partial = partial + mass[part] * shrink
            if d + 1 < chips:
                peak[kind, part] = jnp.broadcast_to(top, (tile, lanes))
                total[kind, part] = jnp.broadcast_to(summed, (tile, lanes))
                mass[part] = partial
            else:
                mass[part] = partial / summed

        def two_tiles(i, carry):
            one_tile(2 * i)
            one_tile(2 * i + 1)
            return carry

        lax.fori_loop(start // 2, stop // 2, two_tiles, 0)

    def forward(d):
        arrive("kz", d)
        send(("kx", d), keys.at[d, mine], keys.at[d, mine], x_peer)
        send(("ka", d), keys.at[d, mine], keys.at[d, side_mine], sibling)

    def forward_other(d):
        arrive("kx", d)
        send(("kb", d), keys.at[d, other], keys.at[d, side_other], sibling)

    for copy in route_loads:
        copy.wait()
    group = experts[0:1, :] // 2
    near = (group + chips - z) % chips
    first_low = experts[0:1, :] % 2 == 0
    gap = logits[0:1, :] - logits[1:2, :]
    first_weight = group_weight[...] / (1.0 + jnp.exp(-gap))
    second_weight = group_weight[...] / (1.0 + jnp.exp(gap))
    low_weight = jnp.where(first_low, first_weight, second_weight)
    high_weight = jnp.where(first_low, second_weight, first_weight)
    line = lax.broadcasted_iota(jnp.int32, (8, count), 0)
    routes[...] = jnp.where(line == 1, low_weight, jnp.where(line == 2, high_weight, 0.0))
    member = jnp.where(line == near, 1.0, 0.0).astype(jnp.bfloat16)
    square_rows = lax.broadcasted_iota(jnp.int32, (count, count), 0)
    square_columns = lax.broadcasted_iota(jnp.int32, (count, count), 1)
    earlier = jnp.where(square_rows < square_columns, 1.0, 0.0).astype(jnp.bfloat16)
    ranks = jnp.dot(member, earlier, preferred_element_type=jnp.float32)
    slot = lax.broadcasted_iota(jnp.int32, (cap, count), 0).astype(jnp.float32)
    for d in range(chips):
        rank = jnp.where(near == d, ranks[d : d + 1, :], -1.0)
        picker[pl.ds(d * cap, cap), :] = jnp.where(slot == rank, 1.0, 0.0).astype(jnp.bfloat16)
    unpicker[...] = dot_nt(unit, picker[...]).astype(jnp.bfloat16)

    arrive("ka", 0)
    attend(0, 0, 0, tiles)
    forward(1)
    attend(0, 1, 0, tiles)
    forward_other(1)
    for d in range(1, chips - 1):
        forward(d + 1)
        arrive("ka", d)
        arrive("kb", d)
        attend(d, 0, 0, tiles)
        forward_other(d + 1)
        attend(d, 1, 0, tiles)

    piece_rows = half
    relay_rows = piece_rows // 2

    def spread_heads(kind, p):
        buffer = (lean_heads, broad_heads)[kind]
        part = pl.ds(p * piece_rows, piece_rows)
        for k, peer in ((0, x_peer), (1, y_peer)):
            send(("h", kind, p, k), buffer.at[0, part], buffer.at[1 + k, part], peer)

    def relay_heads(kind, p):
        buffer = (lean_heads, broad_heads)[kind]
        for k, peer in ((0, y_peer), (1, x_peer)):
            arrive("h", kind, p, k)
            part = pl.ds(p * piece_rows + k * relay_rows, relay_rows)
            send(("h", kind, p, 2 + k), buffer.at[1 + k, part], buffer.at[3, part], peer)

    lean_low = lax.broadcasted_iota(jnp.int32, (count, lanes), 1) < lanes // 2
    last = chips - 1
    arrive("ka", last)
    arrive("kb", last)
    attend(last, 0, 0, tiles)
    for h in range(heads // 2):
        first = lean_mass[pl.ds(2 * h * count, count), :]
        second = lean_mass[pl.ds((2 * h + 1) * count, count), :]
        pair = jnp.where(lean_low, pltpu.roll(first, lanes // 2, 1), second)
        lean_heads[0, :, pl.ds(h * lanes, lanes)] = pair.astype(jnp.bfloat16)
    spread_heads(0, 0)
    spread_heads(0, 1)
    for p in range(2):
        attend(last, 1, p * tiles // 2, (p + 1) * tiles // 2)
        for h in range(heads):
            picked = pl.ds(p * piece_rows * heads + h, piece_rows, stride=heads)
            broad_heads[0, pl.ds(p * piece_rows, piece_rows), pl.ds(h * lanes, lanes)] = broad_mass[
                picked, :
            ].astype(jnp.bfloat16)
        spread_heads(1, p)
        relay_heads(0, p)
    weight_load.wait()
    lean_width, broad_width = lean_heads.shape[2], broad_heads.shape[2]
    squares = [0.0, 0.0]

    def mix(kind, r):
        buffer, acc, span, start = (
            (lean_heads, lean_acc, lean_width, 0),
            (broad_heads, broad_acc, broad_width, 4 * lean_width),
        )[kind]
        part = pl.ds(pl.multiple_of(start + chunks[r] * span, span), span)
        values = buffer[r].astype(jnp.float32)
        squares[kind] = squares[kind] + jnp.sum(values * values, axis=1, keepdims=True)
        gained = (values * mixer_gain[:, part]).astype(jnp.bfloat16)
        product = jnp.dot(gained, weight[part, :], preferred_element_type=jnp.float32)
        if r == 0:
            acc[...] = product
        else:
            acc[...] += product

    mix(0, 0)
    mix(1, 0)
    relay_heads(1, 0)
    mix(0, 1)
    mix(0, 2)
    relay_heads(1, 1)
    for p in range(2):
        arrive("h", 0, p, 2)
        arrive("h", 0, p, 3)
    mix(0, 3)
    mix(1, 1)
    mix(1, 2)
    for p in range(2):
        arrive("h", 1, p, 2)
        arrive("h", 1, p, 3)
    mix(1, 3)
    lean_scale = lax.rsqrt(squares[0] / (4 * lean_width) + epsilon)
    broad_scale = lax.rsqrt(squares[1] / (4 * broad_width) + epsilon)
    values = (
        tokens[...].astype(jnp.float32)
        + lean_acc[...] * lean_scale
        + broad_acc[...] * broad_scale
    )
    stream[...] = values
    scaled[...] = (values * channel_gain[...]).astype(jnp.bfloat16)
    norm = to_row(jnp.sum(values * values, axis=1, keepdims=True))
    norms[0] = jnp.broadcast_to(norm, (8, count))
    for r, peer in ((1, x_peer), (2, y_peer), (3, far_peer)):
        send(("norm", r), norms.at[0], norms.at[r], peer)

    def pick(d):
        return jnp.dot(
            picker[pl.ds(d * cap, cap), :], scaled[...], preferred_element_type=jnp.float32
        ).astype(jnp.bfloat16)

    piece = cap // 2

    def slot_rows(d, r, side=0):
        return rows.at[d, r, pl.ds(side * cap, cap)]

    def spread(d):
        if d:
            arrive("z", d)
        for k in range(2):
            part, rest = pl.ds(k * piece, piece), pl.ds((1 - k) * piece, piece)
            send(("x", d, k), rows.at[d, 0, part], rows.at[d, 1, part], x_peer)
            send(("y", d, k), rows.at[d, 0, rest], rows.at[d, 2, rest], y_peer)
        send(("side", d, 0), slot_rows(d, 0), slot_rows(d, 0, 1), sibling)

    def relay(d):
        for k, axis, peer in ((0, "x", y_peer), (1, "y", x_peer)):
            arrive(axis, d, 0)
            part = pl.ds(k * piece, piece)
            send(("via", d, k), rows.at[d, 1 + k, part], rows.at[d, 3, part], peer)

    def sides(d):
        for r, axis in ((1, "x"), (2, "y")):
            arrive(axis, d, 1)
            send(("side", d, r), slot_rows(d, r), slot_rows(d, r, 1), sibling)

    def last_side(d):
        arrive("via", d, 0)
        arrive("via", d, 1)
        send(("side", d, 3), slot_rows(d, 3), slot_rows(d, 3, 1), sibling)

    def extra_side(d):
        if d:
            arrive("ez", d)
        send(("es", d), extras.at[0, d], extras.at[1, d], sibling)

    def extra_columns(d, line):
        return jnp.concatenate(
            [to_column(extras[side, d][line : line + 1, :])[:cap] for side in range(2)], axis=0
        )

    def project(d):
        last_side(d)
        for r in range(4):
            arrive("side", d, r)
            block = rows[d, r]
            for source, acc in ((gate_w, gate_acc), (up_w, up_acc)):
                product = jnp.dot(block, source[chunks[r]], preferred_element_type=jnp.float32)
                if r == 0:
                    acc[...] = product
                else:
                    acc[...] += product
        arrive("es", d)
        scale = lax.rsqrt(extra_columns(d, 0) / (4 * width) + epsilon)
        gate_value = gate_acc[...] * scale
        up_value = up_acc[...] * scale
        hidden[d, 0] = (gate_value / (1.0 + jnp.exp(-gate_value)) * up_value).astype(jnp.bfloat16)

    def spread_hidden(d):
        for k in range(2):
            part, rest = pl.ds(k * cap, cap), pl.ds((1 - k) * cap, cap)
            send(("hx", d, k), hidden.at[d, 0, part], hidden.at[d, 1, part], x_peer)
            send(("hy", d, k), hidden.at[d, 0, rest], hidden.at[d, 2, rest], y_peer)

    def relay_hidden(d):
        for k, axis, peer in ((0, "hx", y_peer), (1, "hy", x_peer)):
            arrive(axis, d, 0)
            part = pl.ds(k * cap, cap)
            send(("hvia", d, k), hidden.at[d, 1 + k, part], hidden.at[d, 3, part], peer)

    def finish(d):
        arrive("hx", d, 1)
        arrive("hy", d, 1)
        for r in range(4):
            if r == 3:
                arrive("hvia", d, 0)
                arrive("hvia", d, 1)
            product = jnp.dot(hidden[d, r], down_w[chunks[r]], preferred_element_type=jnp.float32)
            if r == 0:
                result[...] = product
            else:
                result[...] += product
        low, high = extra_columns(d, 1), extra_columns(d, 2)
        share = low + (high - low) * core.astype(jnp.float32)
        swap_send[d] = (result[cap:, :] * share[cap:]).astype(jnp.bfloat16)
        send(("swap", d), swap_send.at[d], swap_recv.at[d], sibling)
        kept = result[:cap, :] * share[:cap]
        arrive("swap", d)
        summed = (kept + swap_recv[d].astype(jnp.float32)).astype(jnp.bfloat16)
        if d == 0:
            arrived[pl.ds(0, cap)] = summed
            return
        back[d] = summed
        send(("back", d), back.at[d], arrived.at[pl.ds(d * cap, cap)], behind[d])

    rows[0, 0, pl.ds(0, cap)] = pick(0)
    spread(0)
    for d in range(1, chips):
        going[d] = pick(d)
        send(("z", d), going.at[d], slot_rows(d, 0), ahead[d])
    for r in range(1, 4):
        arrive("norm", r)
    norm_total = norms[0] + norms[1] + norms[2] + norms[3]
    table = jnp.where(line == 0, norm_total, routes[...])
    table_high = table.astype(jnp.bfloat16)
    table_low = (table - table_high.astype(jnp.float32)).astype(jnp.bfloat16)
    for d in range(chips):
        chosen = picker[pl.ds(d * cap, cap), :]
        picked = dot_nt(table_high, chosen) + dot_nt(table_low, chosen)
        picked = jnp.concatenate([picked, jnp.zeros((8, lanes - cap), jnp.float32)], axis=1)
        if d == 0:
            extras[0, 0] = picked
        else:
            norms_d = extras.at[2, d]
            extras[2, d] = picked
            send(("ez", d), norms_d, extras.at[0, d], ahead[d])
    extra_side(0)
    relay(0)
    spread(1)
    sides(0)
    extra_side(1)
    relay(1)
    spread(2)
    sides(1)
    for copy in gate_loads:
        copy.wait()
    project(0)
    relay(2)
    spread(3)
    sides(2)
    extra_side(2)
    project(1)
    spread_hidden(1)
    relay(3)
    sides(3)
    extra_side(3)
    project(2)
    relay_hidden(1)
    spread_hidden(2)
    project(3)
    relay_hidden(2)
    spread_hidden(3)
    down_load.wait()
    finish(1)
    relay_hidden(3)
    spread_hidden(0)
    finish(2)
    relay_hidden(0)
    finish(3)
    finish(0)
    for d in range(1, chips):
        arrive("back", d)
    final = jnp.dot(unpicker[...], arrived[...], preferred_element_type=jnp.float32)
    out_ref[...] = (stream[...] + final).astype(jnp.bfloat16)
    for copy in pending:
        copy.wait_send()


def rope_tables(sequence, count, heads, lean_size, broad_size):
    def angles(size):
        quarter = size // 4
        steps = np.arange(quarter, dtype=np.float32) / np.float32(quarter)
        frequency = np.float32(theta_base) ** (-steps)
        grid_rows = np.arange(sequence // GRID_W, dtype=np.float32)[:, None] * frequency
        grid_columns = np.arange(GRID_W, dtype=np.float32)[:, None] * frequency
        return grid_rows, grid_columns

    shards, per_shard = sequence // count, count // GRID_W
    row_angles, column_angles = angles(lean_size)
    lean_columns = np.tile(column_angles.T, (1, per_shard))
    lean_rows = np.repeat(row_angles, GRID_W, axis=0).reshape(shards, count, -1).transpose(0, 2, 1)
    lean = [
        np.concatenate([np.cos(lean_rows), np.sin(lean_rows)], axis=1),
        np.concatenate([np.cos(lean_columns), np.sin(lean_columns)], axis=0),
    ]
    row_angles, column_angles = angles(broad_size)

    def both(angle, first):
        blank = np.zeros_like(angle)
        cosine = [np.cos(angle), np.cos(angle)]
        sine = [-np.sin(angle), np.sin(angle)]
        rest = [blank, blank]
        parts = cosine + rest + sine + rest if first else rest + cosine + rest + sine
        return np.concatenate(parts, axis=1)

    broad_rows = both(row_angles, True).reshape(shards, per_shard, -1)
    broad_columns = np.repeat(both(column_angles, False), heads, axis=0)
    broad_columns = broad_columns.reshape(-1, 2, broad_size).transpose(1, 0, 2)
    return [table.astype(np.float32) for table in lean + [broad_rows, broad_columns]]


def paired_layer(
    chips,
    tokens,
    lean,
    lean_gains,
    broad,
    broad_gains,
    mixer_gain,
    output_weight,
    channel_gain,
    expert_weights,
    route_experts,
    route_logits,
    group_weight,
):
    count, width = tokens.shape
    heads, lean_size = lean[0].shape[1:]
    key_heads = lean[1].shape[1]
    broad_size = broad[0].shape[2]
    gate_weight, up_weight, down_weight = expert_weights
    ff = gate_weight.shape[1]
    cap = count // 2
    sequence = count * lax.axis_size("sp")
    tables = rope_tables(sequence, count, heads, lean_size, broad_size)
    operands = (
        [jnp.transpose(part, (1, 2, 0)) for part in lean]
        + [part.reshape(-1, broad_size) for part in broad]
        + [lean_gains, broad_gains]
        + [jnp.asarray(table) for table in tables]
        + [
            jnp.transpose(route_experts),
            jnp.transpose(route_logits),
            group_weight[None, :],
            mixer_gain[None, :],
            tokens,
            channel_gain[None, :],
            output_weight,
            gate_weight.reshape(4, width, ff),
            up_weight.reshape(4, width, ff),
            down_weight.reshape(4, ff, width),
        ]
    )
    landing = [part for part in operands]
    landing[8] = tables[0][0]
    landing[10] = tables[2][0]
    f32, bf16 = jnp.float32, jnp.bfloat16
    return pl.pallas_call(
        functools.partial(layer_kernel, chips),
        out_shape=jax.ShapeDtypeStruct((count, width), bf16),
        in_specs=[pl.BlockSpec(memory_space=pl.ANY)] * len(operands),
        out_specs=pl.BlockSpec(memory_space=pltpu.VMEM),
        scratch_shapes=[pltpu.VMEM(part.shape, part.dtype) for part in landing]
        + [
            pltpu.VMEM((2, count * key_heads, 128), f32),
            pltpu.VMEM((count, 384), bf16),
            pltpu.VMEM((chips, 2 * count, 384), bf16),
            pltpu.VMEM((2, count * heads, 128), bf16),
            pltpu.VMEM((2, count * heads, 128), f32),
            pltpu.VMEM((2, count * heads, 128), f32),
            pltpu.VMEM((count * heads, 128), f32),
            pltpu.VMEM((count * heads, 128), f32),
            pltpu.VMEM((4, count, heads * lean_size), bf16),
            pltpu.VMEM((4, count, heads * broad_size), bf16),
            pltpu.VMEM((count, width), f32),
            pltpu.VMEM((count, width), f32),
            pltpu.VMEM((count, width), f32),
            pltpu.VMEM((count, width), bf16),
            pltpu.VMEM((chips * cap, count), bf16),
            pltpu.VMEM((count, chips * cap), bf16),
            pltpu.VMEM((8, count), f32),
            pltpu.VMEM((4, 8, count), f32),
            pltpu.VMEM((3, chips, 8, 128), f32),
            pltpu.VMEM((chips, cap, width), bf16),
            pltpu.VMEM((chips, 4, 2 * cap, width), bf16),
            pltpu.VMEM((2 * cap, ff), f32),
            pltpu.VMEM((2 * cap, ff), f32),
            pltpu.VMEM((chips, 4, 2 * cap, ff), bf16),
            pltpu.VMEM((2 * cap, width), f32),
            pltpu.VMEM((chips, cap, width), bf16),
            pltpu.VMEM((chips, cap, width), bf16),
            pltpu.VMEM((chips, cap, width), bf16),
            pltpu.VMEM((chips * cap, width), bf16),
            pltpu.SemaphoreType.DMA((len(operands),)),
            pltpu.SemaphoreType.DMA((COPIES,)),
            pltpu.SemaphoreType.DMA((COPIES,)),
        ],
        compiler_params=pltpu.CompilerParams(
            collective_id=0, has_side_effects=True, vmem_limit_bytes=60 * 1024 * 1024
        ),
    )(*operands)


def on_device(
    tokens,
    lean_query,
    lean_key,
    lean_value,
    lean_gains,
    broad_query,
    broad_key,
    broad_value,
    broad_gains,
    mixer_gain,
    output_weight,
    channel_gain,
    gate_weight,
    up_weight,
    down_weight,
    route_experts,
    route_logits,
    group_weight,
):
    row_count = tokens.shape[0]
    positions = lax.axis_index("sp") * row_count + jnp.arange(row_count, dtype=jnp.int32)
    lane_index = lax.axis_index("tp")
    logit_gap = route_logits[:, 0] - route_logits[:, 1]
    weights = group_weight[:, None] * jax.nn.sigmoid(jnp.stack([logit_gap, -logit_gap], axis=1))
    chips = lax.axis_size("sp") // 2
    if (
        lax.axis_size("tp") == 4
        and chips == GROUPS
        and chips == 4
        and route_experts.shape[1] == 2
        and lean_query.shape[1:] == (4, 64)
        and broad_query.shape[1:] == (4, 128)
        and lean_key.shape[1:] == (2, 64)
        and broad_key.shape[1:] == (2, 128)
        and row_count % GRID_W == 0
    ):
        return paired_layer(
            chips,
            tokens,
            (lean_query, lean_key, lean_value),
            lean_gains,
            (broad_query, broad_key, broad_value),
            broad_gains,
            mixer_gain,
            output_weight,
            channel_gain,
            (gate_weight[0], up_weight[0], down_weight[0]),
            route_experts,
            route_logits,
            group_weight,
        )
    lean_queries, lean_keys, lean_values = own_heads(
        lean_query, lean_key, lean_value, lean_gains, positions, lane_index, HQ_A // KV_A
    )
    broad_queries, broad_keys, broad_values = own_heads(
        broad_query, broad_key, broad_value, broad_gains, positions, lane_index, HQ_B // KV_B
    )
    shard_rows = (
        lax.all_gather(lean_keys, "sp", axis=0, tiled=True),
        lax.all_gather(lean_values, "sp", axis=0, tiled=True),
        lax.all_gather(broad_keys, "sp", axis=0, tiled=True),
        lax.all_gather(broad_values, "sp", axis=0, tiled=True),
    )
    lean_state = attend_piece(start_state(lean_queries), lean_queries, shard_rows[0], shard_rows[1])
    broad_state = attend_piece(
        start_state(broad_queries), broad_queries, shard_rows[2], shard_rows[3]
    )
    lean_all, broad_all = (
        lax.all_gather(finish_heads(lean_state), "tp", axis=1, tiled=True),
        lax.all_gather(finish_heads(broad_state), "tp", axis=1, tiled=True),
    )
    lean_width = lean_all.shape[1]
    stream = tokens.astype(jnp.float32) + jnp.dot(
        group_norm(lean_all, mixer_gain[:lean_width]),
        output_weight[:lean_width],
        preferred_element_type=jnp.float32,
    )
    stream = stream + jnp.dot(
        group_norm(broad_all, mixer_gain[lean_width:]),
        output_weight[lean_width:],
        preferred_element_type=jnp.float32,
    )
    squares = lax.psum(jnp.sum(stream * stream, axis=1), "tp")
    normed = (stream * lax.rsqrt(squares / D + epsilon)[:, None] * channel_gain).astype(
        jnp.bfloat16
    )
    experts = lax.axis_size("sp")
    capacity = row_count // (experts // GROUPS)
    flat_experts = route_experts.reshape(-1)
    onehot = (flat_experts[:, None] == jnp.arange(experts, dtype=jnp.int32)[None, :]).astype(
        jnp.int32
    )
    slot_rank = jnp.sum((jnp.cumsum(onehot, axis=0) - 1) * onehot, axis=1)
    slot_index = flat_experts * capacity + slot_rank
    token_owner = jnp.repeat(jnp.arange(row_count, dtype=jnp.int32), route_experts.shape[1])
    filled = jnp.zeros((experts * capacity,), jnp.int32).at[slot_index].set(token_owner + 1)
    slot_live = (filled > 0)[:, None]
    source = jnp.maximum(filled - 1, 0)
    outgoing = jnp.where(slot_live, normed[source], jnp.zeros((), jnp.bfloat16)).reshape(
        experts, capacity, -1
    )
    arrived = lax.all_to_all(outgoing, "sp", split_axis=0, concat_axis=0, tiled=True)
    sources = arrived.shape[0]
    item_count = arrived.shape[1]
    shard_rows = lax.all_gather(arrived, "tp", axis=2, tiled=True)
    flat_rows = shard_rows.reshape(sources * item_count, shard_rows.shape[2])
    gate_part = gate_weight[0]
    up_part = up_weight[0]
    gate_value = jnp.dot(flat_rows, gate_part, preferred_element_type=jnp.float32)
    up_value = jnp.dot(flat_rows, up_part, preferred_element_type=jnp.float32)
    hidden = (jax.nn.silu(gate_value) * up_value).astype(jnp.bfloat16)
    down_part = down_weight[0]
    result = jnp.dot(
        lax.all_gather(hidden, "tp", axis=1, tiled=True),
        down_part,
        preferred_element_type=jnp.float32,
    )
    result = result.astype(jnp.bfloat16).reshape(sources, item_count, -1)
    returned = lax.all_to_all(result, "sp", split_axis=0, concat_axis=0, tiled=True)
    picked = (
        returned.reshape(experts * capacity, -1)[slot_index]
        .reshape(row_count, route_experts.shape[1], -1)
        .astype(jnp.float32)
    )
    return (stream + jnp.sum(picked * weights[:, :, None], axis=1)).astype(jnp.bfloat16)


def solution(mesh):
    return jax.shard_map(
        on_device,
        mesh=mesh,
        in_specs=(
            P("sp", "tp"),
            P("sp", "tp", None),
            P("sp", None, None),
            P("sp", None, None),
            P(),
            P("sp", "tp", None),
            P("sp", None, None),
            P("sp", None, None),
            P(),
            P(),
            P(None, "tp"),
            P("tp"),
            P("sp", None, "tp"),
            P("sp", None, "tp"),
            P("sp", None, "tp"),
            P("sp", None),
            P("sp", None),
            P("sp"),
        ),
        out_specs=P("sp", "tp"),
        check_vma=False,
    )
```
